32 devices in a mesh: ep: 8 (over z, x), tp: 4 (over y, core).
Axes of the slice: x: 2, y: 2, z: 4, core: 2. Of those that a mesh axis runs over, the one named last changes fastest.
Arguments:
- queries: bfloat16 [2048, 2048], P('ep', 'tp'), may hold values from -9 to 9
- key_rows: bfloat16 [2048, 2048], P('ep', 'tp'), may hold values from -9 to 9
- values: bfloat16 [2048, 2048], P('ep', 'tp'), may hold values from -6 to 6
- second_scale: float32 [16], P('tp'), may hold values from 0.3 to 0.8
- head_gain: float32 [128], replicated, may hold values from 0.1 to 1.9
- out_weight: bfloat16 [2048, 2048], P(None, 'tp'), may hold values from -0.125 to 0.125
- routed_in: bfloat16 [2048, 2048], P('ep'), may hold values from -6 to 6
- routed_gain: float32 [2048], replicated, may hold values from 0.1 to 1.9
- expert_ids: int32 [2048, 2], P('ep'), may hold values from 0 to 7, all different within a row; in each aligned block of 256 rows (0 to 255, 256 to 511, ...) at most 128 rows name the same one
- group_logits: float32 [2048, 2], P('ep'), may hold values from -6 to 6
- inner_logits: float32 [2048, 2], P('ep'), may hold values from -6 to 6
- gate_weight: bfloat16 [8, 2048, 4096], P('ep', None, 'tp'), may hold values from -0.125 to 0.125
- up_weight: bfloat16 [8, 2048, 4096], P('ep', None, 'tp'), may hold values from -0.125 to 0.125
- down_weight: bfloat16 [8, 4096, 2048], P('ep', 'tp'), may hold values from -0.09375 to 0.09375
Outputs:
- mixer_out: bfloat16 [2048, 2048], P('ep', 'tp')
- routed_out: bfloat16 [2048, 2048], P('ep', 'tp')
The draws below stay inside these ranges and needn't reach their ends.
Inputs may be any that keep to these rules, and one draw needn't show every extreme that they name: `expert_ids`: the two ids of a row differ. In the rows of one device (aligned blocks of 256 rows) no expert is named by more than 128 rows, a bound that some block reaches.
All inputs are finite; a program needn't handle non-finite values.
Results may differ from the reference program's by a relative error of at most 0.018.
Values may be sent and summed in bfloat16 or wider, within the bound.
No kernel may reach another device: no remote copies, remote signals or barrier semaphores. Data moves between devices by JAX's collectives and lax.ppermute only.
A program may use at most 128 MiB of HBM per device.

```python
import math
import jax
import jax.numpy as jnp
import numpy as np
from jax import lax

D = 2048
HEADS = 16
QK = 64
VD = 128
FF = 4096
TOPK = 2
GROUP_SIZE = 4
TM = 256
LA = 2048
TOKM = 2048
EXPERTS = 8
GROUPS = 2
CAP = 128
N_EP = 8
N_TP = 4


def base_field(key):
    spread = 1.32
    return jnp.clip(jax.random.normal(key, (LA, HEADS * 2 * QK), jnp.float32) * spread, -8.0, 8.0)


def draw_queries(key, part):
    field = base_field(jax.random.fold_in(key, 1))
    return field.astype(jnp.bfloat16)


def draw_key_rows(key, part):
    field = base_field(jax.random.fold_in(key, 2))
    return field.astype(jnp.bfloat16)


def level_of(key, dims, cuts, low, high):
    level, own = 1.0, jax.random.fold_in(key, 6)
    for axis_at, blocks in cuts:
        heights = jnp.exp(jax.random.uniform(jax.random.fold_in(own, axis_at), (blocks,), jnp.float32, low / len(cuts), high / len(cuts)))
        level = level * jnp.repeat(heights, dims[axis_at] // blocks).reshape([-1 if axis == axis_at else 1 for axis in range(len(dims))])
    return level


def shared_out(rng, own, number, rows, amount, top, most, slope):
    sequence = jax.random.permutation(rng, amount)
    heavy_load, ordinary = load_shares(amount, rows * top, most, slope, True), load_shares(amount, rows * top, most, slope, False)
    places = jnp.arange(amount)

    def named(tallies, rotation):
        used = int((tallies > 0).sum())
        fixed = max(1, used // 4)
        moved = fixed + (places - fixed + rotation * (used - fixed)) % max(1, amount - fixed)
        return jnp.zeros((amount,), jnp.int32).at[sequence[jnp.where(places < fixed, places, moved)]].set(jnp.asarray(tallies, jnp.int32))

    tallies = jnp.where(number % 4 == 0, named(heavy_load, number // 4), named(ordinary, number - number // 4 - 1))
    mixed = jax.random.permutation(jax.random.fold_in(own, 3), amount)
    donor, taker = mixed[0:amount // 2 * 2:2], mixed[1:amount // 2 * 2:2]
    room = jnp.minimum(tallies[donor] - 1, most - tallies[taker]) // 2
    room = jnp.where((donor == sequence[0]) | (taker == sequence[0]) | (tallies[taker] == 0), 0, jnp.maximum(room, 0))
    moved = jax.random.randint(jax.random.fold_in(own, 4), (amount // 2,), 0, 1 << 20) % (room + 1)
    tallies = tallies.at[donor].add(-moved).at[taker].add(moved)
    items = jnp.searchsorted(jnp.cumsum(tallies), jnp.arange(rows * top), side="right").astype(jnp.int32)
    listing = items.reshape(top, rows).T
    listing = listing[jax.random.permutation(jax.random.fold_in(own, 1), rows)]
    rotation = jax.random.randint(jax.random.fold_in(own, 2), (rows, 1), 0, top)
    return jnp.take_along_axis(listing, (jnp.arange(top)[None, :] + rotation) % top, axis=1)


def load_shares(number_of, total, reach, skew, full):
    loads = [(1 << 20) // math.isqrt(standing ** skew) + 1 for standing in range(1, number_of + 1)]
    largest = reach if full else min(reach, max(-(-total // number_of), total * loads[0] // sum(loads)))
    least = 1 if total - largest >= number_of - 1 else 0
    given, surplus = [largest] + [least] * (number_of - 1), total - largest - least * (number_of - 1)
    while surplus > 0:
        free = [i for i in range(1, number_of) if given[i] < largest] or [i for i in range(1, number_of) if given[i] < reach]
        whole, budget = sum([loads[i] for i in free]), surplus
        for i in free:
            addition = min(reach - given[i], max(1, budget * loads[i] // whole), surplus)
            given[i] = given[i] + addition
            surplus = surplus - addition
    return np.array(given)


def gaussian(own_key, extent, width, bound, pieces=(), held_as=jnp.bfloat16):
    entries = jax.random.normal(own_key, extent, jnp.float32) * width
    if len(pieces) > 0:
        entries = level_of(own_key, extent, pieces, -0.22, 0.18) * entries
    return jnp.clip(entries, min=-bound, max=bound).astype(held_as)


def setup_inputs(seed: int = 0) -> dict:
    seeds = jax.random.split(jax.random.key(seed), 15)
    queries = draw_queries(jax.random.fold_in(seeds[14], 71), 0)
    key_rows = draw_key_rows(jax.random.fold_in(seeds[14], 71), 0)
    values = gaussian(seeds[2], (LA, HEADS * VD), 1.0, 6.0, ((0, 8), (1, 4)))
    second_scale = jnp.clip(0.3 + 0.5 * jax.random.uniform(seeds[3], (HEADS,), jnp.float32) ** level_of(seeds[3], (HEADS,), ((0, 4),), -0.2, 0.2), 0.3, 0.8)
    head_gain = jnp.clip(1.0 + 0.18 * jax.random.normal(seeds[4], (VD,), jnp.float32), 0.1, 1.9)
    out_weight = gaussian(seeds[5], (HEADS * VD, D), (HEADS * VD) ** -0.5, 0.125, ((1, 4),))
    routed_in = gaussian(seeds[6], (TOKM, D), 1.0, 6.0, ((0, 8),))
    routed_gain = jnp.clip(1.0 + 0.18 * jax.random.normal(seeds[7], (D,), jnp.float32), 0.1, 1.9)
    expert_ids_keys = jax.random.split(jax.random.fold_in(seeds[8], 1), TOKM // TM)
    expert_ids_turns = jax.random.permutation(jax.random.fold_in(seeds[8], 3), TOKM // TM)
    expert_ids = jax.vmap(lambda own, number: shared_out(jax.random.fold_in(seeds[8], 2), own, number, TM, EXPERTS, TOPK, CAP, 2))(expert_ids_keys, expert_ids_turns).reshape((TOKM, TOPK))
    group_logits = gaussian(seeds[9], (TOKM, GROUPS), 1.5, 6.0, ((0, 8),), jnp.float32)
    inner_logits = gaussian(seeds[10], (TOKM, TOPK), 1.0, 6.0, ((0, 8),), jnp.float32)
    gate_weight = gaussian(seeds[11], (EXPERTS, D, FF), D ** -0.5, 0.125, ((0, 8), (2, 4)))
    up_weight = gaussian(seeds[12], (EXPERTS, D, FF), D ** -0.5, 0.125, ((0, 8), (2, 4)))
    down_weight = gaussian(seeds[13], (EXPERTS, FF, D), FF ** -0.5, 0.09375, ((0, 8), (1, 4)))
    return {"queries": queries, "key_rows": key_rows, "values": values, "second_scale": second_scale, "head_gain": head_gain, "out_weight": out_weight, "routed_in": routed_in, "routed_gain": routed_gain, "expert_ids": expert_ids, "group_logits": group_logits, "inner_logits": inner_logits, "gate_weight": gate_weight, "up_weight": up_weight, "down_weight": down_weight}


EPSILON = 1e-05

def head_block(query_block, key_block, value_block, scale_head, first_pos):
    scores = jnp.einsum('qmd,kmd->mqk', query_block, key_block) * QK ** (-0.5)
    query_pos = first_pos + jnp.arange(query_block.shape[0], dtype=jnp.int32)
    key_pos = jnp.arange(key_block.shape[0], dtype=jnp.int32)
    visible = query_pos[:, None] >= key_pos[None, :]
    scores = jnp.where(visible, scores, -jnp.inf)
    row_max = lax.optimization_barrier(jnp.max(scores, axis=-1, keepdims=True))
    exp_terms = jnp.exp(scores - row_max)
    denominator = lax.optimization_barrier(jnp.sum(exp_terms, axis=-1))
    rounded = lax.optimization_barrier(exp_terms.astype(jnp.bfloat16)).astype(jnp.float32)
    weighted = jnp.einsum('mqk,ke->mqe', rounded, value_block)
    mapped = weighted / denominator[..., None]
    return mapped[0] - scale_head * mapped[1]

def reference(queries, key_rows, values, second_scale, head_gain, out_weight, routed_in, routed_gain, expert_ids, group_logits, inner_logits, gate_weight, up_weight, down_weight):
    query_all = jnp.transpose(queries.astype(jnp.float32).reshape(LA, HEADS, 2, QK), (1, 0, 2, 3))
    key_all = jnp.transpose(key_rows.astype(jnp.float32).reshape(LA, HEADS, 2, QK), (1, 0, 2, 3))
    value_all = jnp.transpose(values.astype(jnp.float32).reshape(LA, HEADS, VD), (1, 0, 2))
    block_rows = min(512, LA)
    outputs = []
    for first_pos in range(0, LA, block_rows):
        limit = first_pos + block_rows

        def per_head(operands, first_pos=first_pos):
            query_head, key_head, value_head, scale_head = operands
            return head_block(query_head, key_head, value_head, scale_head, first_pos)
        outputs.append(lax.map(per_head, (query_all[:, first_pos:limit], key_all[:, :limit], value_all[:, :limit], second_scale)))
    difference = jnp.concatenate(outputs, axis=1)
    inv_norm = lax.rsqrt(lax.optimization_barrier(jnp.mean(difference * difference, axis=-1, keepdims=True)) + EPSILON)
    head_out = (difference * inv_norm * head_gain).astype(jnp.bfloat16)
    head_out = jnp.transpose(head_out, (1, 0, 2)).reshape(LA, HEADS * VD)
    mixer_out = jnp.dot(head_out, out_weight, preferred_element_type=jnp.float32).astype(jnp.bfloat16)
    source = routed_in.astype(jnp.float32)
    normed = (source * lax.rsqrt(lax.optimization_barrier(jnp.mean(source * source, axis=-1, keepdims=True)) + EPSILON) * routed_gain).astype(jnp.bfloat16)
    block_ids = expert_ids.reshape(N_EP, TM * TOPK)
    picked = (block_ids[..., None] == jnp.arange(EXPERTS, dtype=jnp.int32)).astype(jnp.int32)
    slot_index = lax.optimization_barrier(jnp.sum(jnp.cumsum(picked, axis=1) * picked, axis=-1)) - 1
    place_index = (jnp.arange(N_EP, dtype=jnp.int32)[:, None] * CAP + slot_index).reshape(-1).astype(jnp.int32)
    flat_ids = expert_ids.reshape(-1).astype(jnp.int32)
    owner_row = (jnp.arange(TOKM * TOPK, dtype=jnp.int32) // TOPK).astype(jnp.int32)
    slot_rows = jnp.zeros((EXPERTS, N_EP * CAP), jnp.int32).at[flat_ids, place_index].set(owner_row)

    def one_expert(operands):
        rows_of, gate_part, up_part, down_part = operands
        gathered = normed[rows_of]
        gate_act = jnp.dot(gathered, gate_part, preferred_element_type=jnp.float32)
        up_act = jnp.dot(gathered, up_part, preferred_element_type=jnp.float32)
        hidden = (jax.nn.silu(gate_act) * up_act).astype(jnp.bfloat16)
        split_hidden = hidden.reshape(N_EP * CAP, N_TP, FF // N_TP).astype(jnp.float32)
        split_down = down_part.reshape(N_TP, FF // N_TP, D).astype(jnp.float32)
        partial_value = jnp.einsum('rtf,tfd->trd', split_hidden, split_down)
        rounded = lax.optimization_barrier(partial_value.astype(jnp.bfloat16)).astype(jnp.float32)
        return lax.optimization_barrier(jnp.sum(rounded, axis=0)).astype(jnp.bfloat16)
    expert_out = lax.map(one_expert, (slot_rows, gate_weight, up_weight, down_weight))
    pair_out = expert_out[flat_ids, place_index].reshape(TOKM, TOPK, D)
    group_prob = jax.nn.softmax(group_logits, axis=-1)
    member = (expert_ids[..., None] // GROUP_SIZE == jnp.arange(GROUPS, dtype=jnp.int32)).astype(jnp.float32)
    group_pick = lax.optimization_barrier(jnp.sum(group_prob[:, None, :] * member, axis=-1))
    route_weight = group_pick * jax.nn.softmax(inner_logits, axis=-1)
    routed_out = lax.optimization_barrier(jnp.sum(route_weight[..., None] * pair_out.astype(jnp.float32), axis=1)).astype(jnp.bfloat16)
    return (mixer_out, routed_out)
```

```python
import functools

import jax
import jax.numpy as jnp
from jax import lax
from jax.experimental import pallas as pl
from jax.experimental.pallas import tpu as pltpu
from jax.sharding import PartitionSpec as P

GROUP_SIZE = 4
EPSILON = 1e-05
LOWEST = -1e30


VMEM = pl.BlockSpec(memory_space=pltpu.VMEM)
SMEM = pl.BlockSpec(memory_space=pltpu.SMEM)


def dot32(a, b):
    return jnp.dot(a, b, preferred_element_type=jnp.float32)


def shift(x, by):
    n = lax.axis_size("ep")
    return lax.ppermute(x, "ep", [(i, (i + by) % n) for i in range(n)])


def pair_swap(x):
    n = lax.axis_size("ep")
    return lax.ppermute(x, "ep", [(i, i ^ 1) for i in range(n)])


def pair_up(x):
    n = lax.axis_size("ep")
    return lax.ppermute(x, "ep", [(i, i + 2) for i in range(n - 2)])


def tp_swap(x, bit):
    n = lax.axis_size("tp")
    return lax.ppermute(x, "tp", [(i, i ^ bit) for i in range(n)])


def tp_bits():
    n = lax.axis_size("tp")
    return [1 << b for b in reversed(range(n.bit_length() - 1))]


def tp_pieces(x):
    pieces = [x]
    for bit in tp_bits():
        pieces += [tp_swap(piece, bit) for piece in pieces]
    return pieces


def tp_order():
    t = lax.axis_index("tp").astype(jnp.int32)
    order = [t]
    for bit in tp_bits():
        order += [part ^ bit for part in order]
    return jnp.stack(order)


def add_shares(send, keep):
    got = tp_swap(send, 1)
    sums = [
        keep[j].astype(jnp.float32) + got[j].astype(jnp.float32) for j in range(keep.shape[0])
    ]
    bit = 2 * len(sums)
    while len(sums) > 1:
        bit //= 2
        middle = len(sums) // 2
        far = [tp_swap(part.astype(jnp.bfloat16), bit) for part in sums[middle:]]
        sums = [part + other.astype(jnp.float32) for part, other in zip(sums[:middle], far)]
    return sums[0].astype(jnp.bfloat16)


def attention_kernel(blocks, valid, scale_ref, gain_ref, q_ref, *refs):
    keys, vals = refs[:blocks], refs[blocks : 2 * blocks]
    out_ref, s_ref, m_ref, l_ref, acc_ref = refs[2 * blocks :]
    rows, width = q_ref.shape
    half = width // 2
    lane = lax.broadcasted_iota(jnp.int32, (rows, width), 1)
    q = q_ref[...] * jnp.asarray(half ** (-0.5), q_ref.dtype)
    zero = jnp.zeros_like(q)
    both = jnp.concatenate([jnp.where(lane < half, q, zero), jnp.where(lane >= half, q, zero)], axis=0)

    def scores(p):
        return lax.dot_general(
            both, keys[p][...], (((1,), (1,)), ((), ())), preferred_element_type=jnp.float32
        )

    count = keys[0].shape[0]
    row = lax.broadcasted_iota(jnp.int32, (2 * rows, count), 0)
    row = jnp.where(row >= rows, row - rows, row)
    col = lax.broadcasted_iota(jnp.int32, (2 * rows, count), 1)
    first = jnp.where(row >= col, scores(0), LOWEST)
    s_ref[0] = first
    m_ref[...] = jnp.broadcast_to(jnp.max(first, axis=1, keepdims=True), m_ref.shape)
    for p in range(1, blocks):

        @pl.when(valid[p] > 0)
        def _(p=p):
            s = scores(p)
            s_ref[p] = s
            m_ref[...] = jnp.maximum(m_ref[...], jnp.max(s, axis=1, keepdims=True))

    def terms(p):
        e = jnp.exp(s_ref[p] - m_ref[:, :1])
        return jnp.sum(e, axis=1, keepdims=True), dot32(e.astype(jnp.bfloat16), vals[p][...])

    total, weighted = terms(0)
    l_ref[...] = jnp.broadcast_to(total, l_ref.shape)
    acc_ref[...] = weighted
    for p in range(1, blocks):

        @pl.when(valid[p] > 0)
        def _(p=p):
            total, weighted = terms(p)
            l_ref[...] += total
            acc_ref[...] += weighted

    mapped = acc_ref[...] / l_ref[...]
    difference = mapped[:rows] - scale_ref[pl.program_id(0)] * mapped[rows:]
    inv_norm = lax.rsqrt(jnp.mean(difference * difference, axis=1, keepdims=True) + EPSILON)
    out_ref[...] = (difference * inv_norm * gain_ref[...]).astype(out_ref.dtype)


def attend(queries, pieces, valid, second_scale, head_gain):
    rows = queries.shape[0]
    heads = second_scale.shape[0]
    width = queries.shape[1] // heads
    size = head_gain.shape[0]
    count = pieces[0].shape[0]
    blocks = len(pieces)
    offset = queries.shape[1] // size
    grid_spec = pltpu.PrefetchScalarGridSpec(
        num_scalar_prefetch=2,
        grid=(heads,),
        in_specs=[
            pl.BlockSpec((1, size), lambda h, *_: (0, 0)),
            pl.BlockSpec((rows, width), lambda h, *_: (0, h)),
        ]
        + [pl.BlockSpec((count, width), lambda h, *_: (0, h)) for _ in pieces]
        + [pl.BlockSpec((count, size), lambda h, *_: (0, offset + h)) for _ in pieces],
        out_specs=pl.BlockSpec((rows, size), lambda h, *_: (0, h)),
        scratch_shapes=[
            pltpu.VMEM((blocks, 2 * rows, count), jnp.float32),
            pltpu.VMEM((2 * rows, size), jnp.float32),
            pltpu.VMEM((2 * rows, size), jnp.float32),
            pltpu.VMEM((2 * rows, size), jnp.float32),
        ],
    )
    return pl.pallas_call(
        functools.partial(attention_kernel, blocks),
        grid_spec=grid_spec,
        out_shape=jax.ShapeDtypeStruct((rows, heads * size), jnp.bfloat16),
        name="attend",
    )(valid, second_scale, head_gain[None, :], queries, *pieces, *pieces)


def project_kernel(order, weight_ref, *refs):
    parts, out_ref = refs[:-1], refs[-1]
    width = parts[0].shape[1]
    total = None
    for j, part in enumerate(parts):
        at = pl.multiple_of(order[j] * width, width)
        term = dot32(part[...], weight_ref[pl.ds(at, width), :])
        total = term if total is None else total + term
    out_ref[...] = total.astype(out_ref.dtype)


def token_mixer(queries, key_rows, values, second_scale, head_gain, out_weight):
    index = lax.axis_index("ep").astype(jnp.int32)
    pairs = lax.axis_size("ep") // 2
    own = jnp.concatenate([key_rows, values], axis=1)
    pieces = [own, pair_swap(own)]
    block_ids = [index, jnp.where(index % 2 == 1, index - 1, -1)]
    moving = own
    for step in range(1, pairs):
        moving = pair_up(moving)
        pieces += [moving, pair_swap(moving)]
        block_ids += [index - 2 * step, (index ^ 1) - 2 * step]
    valid = (jnp.stack(block_ids) >= 0).astype(jnp.int32)
    head_out = attend(queries, pieces, valid, second_scale, head_gain)
    parts = tp_pieces(head_out)
    return pl.pallas_call(
        project_kernel,
        in_specs=[SMEM, VMEM] + [VMEM] * len(parts),
        out_specs=VMEM,
        out_shape=jax.ShapeDtypeStruct((queries.shape[0], out_weight.shape[1]), jnp.bfloat16),
        name="project",
    )(tp_order(), out_weight, *parts)


def dispatch_kernel(offsets, capacity, tp_index, ids_ref, gain_ref, x_ref, *outs):
    rows = x_ref.shape[0]
    width = outs[0].shape[1]
    experts = len(offsets)
    x = x_ref[...].astype(jnp.float32)
    inv_norm = lax.rsqrt(jnp.mean(x * x, axis=1, keepdims=True) + EPSILON)
    at = pl.multiple_of(tp_index[0] * width, width)
    own = x_ref[:, pl.ds(at, width)].astype(jnp.float32)
    normed = (own * inv_norm * gain_ref[:, pl.ds(at, width)]).astype(jnp.bfloat16)
    expert = lax.broadcasted_iota(jnp.int32, (experts, rows), 0)
    picked = jnp.zeros((experts, rows), jnp.float32)
    for k in range(ids_ref.shape[0]):
        picked += jnp.where(ids_ref[k : k + 1, :] == expert, 1.0, 0.0)
    earlier = lax.broadcasted_iota(jnp.int32, (rows, rows), 0) < lax.broadcasted_iota(
        jnp.int32, (rows, rows), 1
    )
    rank = dot32(picked.astype(jnp.bfloat16), jnp.where(earlier, 1.0, 0.0).astype(jnp.bfloat16))
    slot = jnp.where(picked > 0, rank, -1.0).astype(jnp.int32)
    place = lax.broadcasted_iota(jnp.int32, (capacity, rows), 0)
    for d, out in zip(offsets, outs):
        chosen = jnp.where(place == slot[d : d + 1, :], 1.0, 0.0).astype(jnp.bfloat16)
        out[...] = dot32(chosen, normed).astype(out.dtype)


def expert_kernel(tiles, half, order, dest, *refs):
    parts = refs[: 2 * half]
    gate_ref, up_ref, down_ref, send_ref, keep_ref, x_ref, hidden_ref = refs[2 * half :]
    step = pl.program_id(0)
    width = parts[0].shape[1]
    tile = gate_ref.shape[1]

    @pl.when(step == 0)
    def _():
        for j, part in enumerate(parts):
            x_ref[:, pl.ds(pl.multiple_of(order[j] * width, width), width)] = part[...]

    @pl.when(step < tiles)
    def _():
        gate = dot32(x_ref[...], gate_ref[...])
        up = dot32(x_ref[...], up_ref[...])
        value = (gate / (1.0 + jnp.exp(-gate)) * up).astype(jnp.bfloat16)
        hidden_ref[:, pl.ds(pl.multiple_of(step * tile, tile), tile)] = value

    @pl.when((step >= tiles) & (step < tiles + half))
    def _():
        send_ref[0] = dot32(hidden_ref[...], down_ref[...]).astype(jnp.bfloat16)

    @pl.when(step >= tiles + half)
    def _():
        keep_ref[0] = dot32(hidden_ref[...], down_ref[...]).astype(jnp.bfloat16)


def run_experts(parts, gate_local, up_local, down_local):
    rows, width = parts[0].shape
    model, units = gate_local.shape
    tile = min(units, 256)
    tiles = units // tile
    t = lax.axis_index("tp").astype(jnp.int32)
    half = len(parts) // 2
    dest = jnp.stack([t ^ (2 * j + 1) for j in range(half)] + [t ^ (2 * j) for j in range(half)])
    whole = pl.BlockSpec((rows, width), lambda i, *_: (0, 0))
    column = pl.BlockSpec((model, tile), lambda i, *_: (0, jnp.minimum(i, tiles - 1)))
    grid_spec = pltpu.PrefetchScalarGridSpec(
        num_scalar_prefetch=2,
        grid=(tiles + 2 * half,),
        in_specs=[whole] * (2 * half)
        + [
            column,
            column,
            pl.BlockSpec(
                (units, width), lambda i, order, dest: (0, dest[jnp.maximum(i - tiles, 0)])
            ),
        ],
        out_specs=[
            pl.BlockSpec((1, rows, width), lambda i, *_: (jnp.clip(i - tiles, 0, half - 1), 0, 0)),
            pl.BlockSpec((1, rows, width), lambda i, *_: (jnp.clip(i - tiles - half, 0, half - 1), 0, 0)),
        ],
        scratch_shapes=[
            pltpu.VMEM((rows, model), jnp.bfloat16),
            pltpu.VMEM((rows, units), jnp.bfloat16),
        ],
    )
    shape = jax.ShapeDtypeStruct((half, rows, width), jnp.bfloat16)
    return pl.pallas_call(
        functools.partial(expert_kernel, tiles, half),
        grid_spec=grid_spec,
        out_shape=[shape, shape],
        name="experts",
    )(tp_order(), dest, *parts, gate_local, up_local, down_local)


def combine_kernel(offsets, ids_ref, route_ref, *refs):
    blocks, out_ref = refs[:-1], refs[-1]
    rows, chosen = ids_ref.shape
    experts = len(offsets)
    capacity = blocks[0].shape[0]
    expert = lax.broadcasted_iota(jnp.int32, (rows, experts), 1)
    picked = jnp.zeros((rows, experts), jnp.float32)
    weight = jnp.zeros((rows, experts), jnp.float32)
    for k in range(chosen):
        match = ids_ref[:, k : k + 1] == expert
        picked += jnp.where(match, 1.0, 0.0)
        weight += jnp.where(match, route_ref[:, k : k + 1], 0.0)
    earlier = lax.broadcasted_iota(jnp.int32, (rows, rows), 1) < lax.broadcasted_iota(
        jnp.int32, (rows, rows), 0
    )
    rank = dot32(jnp.where(earlier, 1.0, 0.0).astype(jnp.bfloat16), picked.astype(jnp.bfloat16))
    slot = jnp.where(picked > 0, rank, -1.0).astype(jnp.int32)
    place = lax.broadcasted_iota(jnp.int32, (rows, capacity), 1)
    total = None
    for d, block in zip(offsets, blocks):
        spread = jnp.where(place == slot[:, d : d + 1], weight[:, d : d + 1], 0.0)
        high = spread.astype(jnp.bfloat16)
        low = (spread - high.astype(jnp.float32)).astype(jnp.bfloat16)
        term = dot32(high, block[...]) + dot32(low, block[...])
        total = term if total is None else total + term
    out_ref[...] = total.astype(out_ref.dtype)


def expert_block(
    routed_in,
    routed_gain,
    expert_ids,
    group_logits,
    inner_logits,
    gate_weight,
    up_weight,
    down_weight,
):
    token_count = routed_in.shape[0]
    chosen = expert_ids.shape[1]
    ep_size = lax.axis_size("ep")
    capacity = 2 * chosen * token_count // ep_size
    width = routed_in.shape[1] // lax.axis_size("tp")
    index = lax.axis_index("ep").astype(jnp.int32)
    relative = jnp.where(expert_ids < index, expert_ids - index + ep_size, expert_ids - index)
    offsets = sorted(range(ep_size), key=lambda d: (min(d, ep_size - d), d))
    outgoing = pl.pallas_call(
        functools.partial(dispatch_kernel, offsets, capacity),
        in_specs=[SMEM, VMEM, VMEM, VMEM],
        out_specs=[VMEM] * ep_size,
        out_shape=[jax.ShapeDtypeStruct((capacity, width), jnp.bfloat16)] * ep_size,
        name="dispatch",
    )(
        lax.axis_index("tp").astype(jnp.int32)[None],
        relative.T,
        routed_gain[None, :],
        routed_in,
    )
    arrived = [x if d == 0 else shift(x, d) for d, x in zip(offsets, outgoing)]
    half = ep_size // 2
    returned = []
    for start in range(0, ep_size, half):
        batch = jnp.concatenate(arrived[start : start + half], axis=0)
        send, keep = run_experts(tp_pieces(batch), gate_weight[0], up_weight[0], down_weight[0])
        answered = add_shares(send, keep)
        for j, d in enumerate(offsets[start : start + half]):
            piece = answered[j * capacity : (j + 1) * capacity]
            returned.append(piece if d == 0 else shift(piece, ep_size - d))
    group_prob = jax.nn.softmax(group_logits, axis=-1)
    member = (
        expert_ids[..., None] // GROUP_SIZE == jnp.arange(group_logits.shape[1], dtype=jnp.int32)
    ).astype(jnp.float32)
    group_pick = jnp.sum(group_prob[:, None, :] * member, axis=-1)
    route_weight = group_pick * jax.nn.softmax(inner_logits, axis=-1)
    return pl.pallas_call(
        functools.partial(combine_kernel, offsets),
        in_specs=[VMEM] * (2 + ep_size),
        out_specs=VMEM,
        out_shape=jax.ShapeDtypeStruct((token_count, width), jnp.bfloat16),
        name="combine",
    )(relative, route_weight, *returned)


def local(
    queries,
    key_rows,
    values,
    second_scale,
    head_gain,
    out_weight,
    routed_in,
    routed_gain,
    expert_ids,
    group_logits,
    inner_logits,
    gate_weight,
    up_weight,
    down_weight,
):
    routed_out = expert_block(
        routed_in,
        routed_gain,
        expert_ids,
        group_logits,
        inner_logits,
        gate_weight,
        up_weight,
        down_weight,
    )
    mixer_out = token_mixer(queries, key_rows, values, second_scale, head_gain, out_weight)
    return (mixer_out, routed_out)


def solution(mesh):
    return jax.shard_map(
        local,
        mesh=mesh,
        in_specs=(
            P("ep", "tp"),
            P("ep", "tp"),
            P("ep", "tp"),
            P("tp"),
            P(),
            P(None, "tp"),
            P("ep", None),
            P(),
            P("ep", None),
            P("ep", None),
            P("ep", None),
            P("ep", None, "tp"),
            P("ep", None, "tp"),
            P("ep", "tp", None),
        ),
        out_specs=(P("ep", "tp"), P("ep", "tp")),
        check_vma=False,
    )
```

```python
import functools

import jax
import jax.numpy as jnp
from jax import lax
from jax.experimental import pallas as pl
from jax.experimental.pallas import tpu as pltpu
from jax.sharding import PartitionSpec as P


GROUP_SIZE = 4
EPSILON = 1e-05
LOWEST = -1e30


VMEM = pl.BlockSpec(memory_space=pltpu.VMEM)
SMEM = pl.BlockSpec(memory_space=pltpu.SMEM)


def dot32(a, b):
    return jnp.dot(a, b, preferred_element_type=jnp.float32)


def shift(x, by):
    n = lax.axis_size("ep")
    return lax.ppermute(x, "ep", [(i, (i + by) % n) for i in range(n)])


def pair_swap(x):
    n = lax.axis_size("ep")
    return lax.ppermute(x, "ep", [(i, i ^ 1) for i in range(n)])


def pair_up(x):
    n = lax.axis_size("ep")
    return lax.ppermute(x, "ep", [(i, i + 2) for i in range(n - 2)])


def tp_swap(x, bit):
    n = lax.axis_size("tp")
    return lax.ppermute(x, "tp", [(i, i ^ bit) for i in range(n)])


def tp_bits():
    n = lax.axis_size("tp")
    return [1 << b for b in reversed(range(n.bit_length() - 1))]


def tp_pieces(x):
    pieces = [x]
    for bit in tp_bits():
        pieces += [tp_swap(piece, bit) for piece in pieces]
    return pieces


def tp_order():
    t = lax.axis_index("tp").astype(jnp.int32)
    order = [t]
    for bit in tp_bits():
        order += [part ^ bit for part in order]
    return jnp.stack(order)


def add_shares(send, keep):
    got = tp_swap(send, 1)
    sums = [
        keep[j].astype(jnp.float32) + got[j].astype(jnp.float32) for j in range(keep.shape[0])
    ]
    bit = 2 * len(sums)
    while len(sums) > 1:
        bit //= 2
        middle = len(sums) // 2
        far = [tp_swap(part.astype(jnp.bfloat16), bit) for part in sums[middle:]]
        sums = [part + other.astype(jnp.float32) for part, other in zip(sums[:middle], far)]
    return sums[0].astype(jnp.bfloat16)


def attention_kernel(blocks, first_head, valid, scale_ref, gain_ref, q_ref, *refs):
    keys, vals = refs[:blocks], refs[blocks : 2 * blocks]
    out_ref, s_ref, m_ref, l_ref, acc_ref = refs[2 * blocks :]
    rows, width = q_ref.shape
    half = width // 2
    lane = lax.broadcasted_iota(jnp.int32, (rows, width), 1)
    q = q_ref[...] * jnp.asarray(half ** (-0.5), q_ref.dtype)
    zero = jnp.zeros_like(q)
    both = jnp.concatenate([jnp.where(lane < half, q, zero), jnp.where(lane >= half, q, zero)], axis=0)

    def fold(x, op):
        lanes = m_ref.shape[1]
        return functools.reduce(op, [x[:, c : c + lanes] for c in range(0, x.shape[1], lanes)])

    def scores(p):
        return lax.dot_general(
            both, keys[p][...], (((1,), (1,)), ((), ())), preferred_element_type=jnp.float32
        )

    count = keys[0].shape[0]
    row = lax.broadcasted_iota(jnp.int32, (2 * rows, count), 0)
    row = jnp.where(row >= rows, row - rows, row)
    col = lax.broadcasted_iota(jnp.int32, (2 * rows, count), 1)
    first = jnp.where(row >= col, scores(0), LOWEST)
    s_ref[0] = first
    m_ref[...] = fold(first, jnp.maximum)
    for p in range(1, blocks):

        @pl.when(valid[p] > 0)
        def _(p=p):
            s = scores(p)
            s_ref[p] = s
            m_ref[...] = jnp.maximum(m_ref[...], fold(s, jnp.maximum))

    m_ref[...] = jnp.broadcast_to(jnp.max(m_ref[...], axis=1, keepdims=True), m_ref.shape)

    def terms(p):
        lanes = m_ref.shape[1]
        e = jnp.concatenate(
            [jnp.exp(s_ref[p, :, c : c + lanes] - m_ref[...]) for c in range(0, count, lanes)], axis=1
        )
        return fold(e, jnp.add), dot32(e.astype(jnp.bfloat16), vals[p][...])

    total, weighted = terms(0)
    l_ref[...] = total
    acc_ref[...] = weighted
    for p in range(1, blocks):

        @pl.when(valid[p] > 0)
        def _(p=p):
            total, weighted = terms(p)
            l_ref[...] += total
            acc_ref[...] += weighted

    mapped = acc_ref[...] / jnp.sum(l_ref[...], axis=1, keepdims=True)
    difference = mapped[:rows] - scale_ref[first_head + pl.program_id(0)] * mapped[rows:]
    inv_norm = lax.rsqrt(jnp.mean(difference * difference, axis=1, keepdims=True) + EPSILON)
    out_ref[...] = (difference * inv_norm * gain_ref[...]).astype(out_ref.dtype)


def attend(queries, pieces, valid, second_scale, head_gain, begin, amount):
    rows = queries.shape[0]
    heads = second_scale.shape[0]
    width = queries.shape[1] // heads
    size = head_gain.shape[0]
    count = pieces[0].shape[0]
    blocks = len(pieces)
    offset = queries.shape[1] // size
    grid_spec = pltpu.PrefetchScalarGridSpec(
        num_scalar_prefetch=2,
        grid=(amount,),
        in_specs=[
            pl.BlockSpec((1, size), lambda h, *_: (0, 0)),
            pl.BlockSpec((rows, width), lambda h, *_: (0, begin + h)),
        ]
        + [pl.BlockSpec((count, width), lambda h, *_: (0, begin + h)) for _ in pieces]
        + [pl.BlockSpec((count, size), lambda h, *_: (0, offset + begin + h)) for _ in pieces],
        out_specs=pl.BlockSpec((rows, size), lambda h, *_: (0, h)),
        scratch_shapes=[
            pltpu.VMEM((blocks, 2 * rows, count), jnp.float32),
            pltpu.VMEM((2 * rows, size), jnp.float32),
            pltpu.VMEM((2 * rows, size), jnp.float32),
            pltpu.VMEM((2 * rows, size), jnp.float32),
        ],
    )
    return pl.pallas_call(
        functools.partial(attention_kernel, blocks, begin),
        grid_spec=grid_spec,
        out_shape=jax.ShapeDtypeStruct((rows, amount * size), jnp.bfloat16),
        name="attend",
    )(valid, second_scale, head_gain[None, :], queries, *pieces, *pieces)


def project_kernel(splits, order, weight_ref, *refs):
    parts, out_ref = refs[:-1], refs[-1]
    width = parts[0].shape[1]
    total = None
    for j, part in enumerate(parts):
        split, share = divmod(j, len(parts) // splits)
        at = pl.multiple_of((order[share] * splits + split) * width, width)
        term = dot32(part[...], weight_ref[pl.ds(at, width), :])
        total = term if total is None else total + term
    out_ref[...] = total.astype(out_ref.dtype)


def token_mixer(queries, key_rows, values, second_scale, head_gain, out_weight):
    index = lax.axis_index("ep").astype(jnp.int32)
    pairs = lax.axis_size("ep") // 2
    own = jnp.concatenate([key_rows, values], axis=1)
    pieces = [own, pair_swap(own)]
    block_ids = [index, jnp.where(index % 2 == 1, index - 1, -1)]
    moving = own
    for step in range(1, pairs):
        moving = pair_up(moving)
        pieces += [moving, pair_swap(moving)]
        block_ids += [index - 2 * step, (index ^ 1) - 2 * step]
    valid = (jnp.stack(block_ids) >= 0).astype(jnp.int32)
    heads = second_scale.shape[0]
    splits = 2 if heads % 2 == 0 else 1
    amount = heads // splits
    parts = []
    for split in range(splits):
        head_out = attend(queries, pieces, valid, second_scale, head_gain, split * amount, amount)
        parts += tp_pieces(head_out)
    return pl.pallas_call(
        functools.partial(project_kernel, splits),
        in_specs=[SMEM, VMEM] + [VMEM] * len(parts),
        out_specs=VMEM,
        out_shape=jax.ShapeDtypeStruct((queries.shape[0], out_weight.shape[1]), jnp.bfloat16),
        name="project",
    )(tp_order(), out_weight, *parts)


def dispatch_kernel(offsets, capacity, tp_index, ids_ref, gain_ref, x_ref, *outs):
    rows = x_ref.shape[0]
    width = outs[0].shape[1]
    experts = len(offsets)
    x = x_ref[...].astype(jnp.float32)
    inv_norm = lax.rsqrt(jnp.mean(x * x, axis=1, keepdims=True) + EPSILON)
    at = pl.multiple_of(tp_index[0] * width, width)
    own = x_ref[:, pl.ds(at, width)].astype(jnp.float32)
    normed = (own * inv_norm * gain_ref[:, pl.ds(at, width)]).astype(jnp.bfloat16)
    expert = lax.broadcasted_iota(jnp.int32, (experts, rows), 0)
    picked = jnp.zeros((experts, rows), jnp.float32)
    for k in range(ids_ref.shape[0]):
        picked += jnp.where(ids_ref[k : k + 1, :] == expert, 1.0, 0.0)
    earlier = lax.broadcasted_iota(jnp.int32, (rows, rows), 0) < lax.broadcasted_iota(
        jnp.int32, (rows, rows), 1
    )
    rank = dot32(picked.astype(jnp.bfloat16), jnp.where(earlier, 1.0, 0.0).astype(jnp.bfloat16))
    slot = jnp.where(picked > 0, rank, -1.0).astype(jnp.int32)
    place = lax.broadcasted_iota(jnp.int32, (capacity, rows), 0)
    for d, out in zip(offsets, outs):
        chosen = jnp.where(place == slot[d : d + 1, :], 1.0, 0.0).astype(jnp.bfloat16)
        out[...] = dot32(chosen, normed).astype(out.dtype)


def expert_kernel(tiles, half, order, dest, *refs):
    parts = refs[: 2 * half]
    gate_ref, up_ref, down_ref, send_ref, keep_ref, x_ref, hidden_ref = refs[2 * half :]
    step = pl.program_id(0)
    width = parts[0].shape[1]
    tile = gate_ref.shape[1]

    @pl.when(step == 0)
    def _():
        for j, part in enumerate(parts):
            x_ref[:, pl.ds(pl.multiple_of(order[j] * width, width), width)] = part[...]

    @pl.when(step < tiles)
    def _():
        gate = dot32(x_ref[...], gate_ref[...])
        up = dot32(x_ref[...], up_ref[...])
        value = (gate / (1.0 + jnp.exp(-gate)) * up).astype(jnp.bfloat16)
        hidden_ref[:, pl.ds(pl.multiple_of(step * tile, tile), tile)] = value

    @pl.when((step >= tiles) & (step < tiles + half))
    def _():
        send_ref[0] = dot32(hidden_ref[...], down_ref[...]).astype(jnp.bfloat16)

    @pl.when(step >= tiles + half)
    def _():
        keep_ref[0] = dot32(hidden_ref[...], down_ref[...]).astype(jnp.bfloat16)


def run_experts(parts, gate_local, up_local, down_local):
    rows, width = parts[0].shape
    model, units = gate_local.shape
    tile = min(units, 256)
    tiles = units // tile
    t = lax.axis_index("tp").astype(jnp.int32)
    half = len(parts) // 2
    dest = jnp.stack([t ^ (2 * j + 1) for j in range(half)] + [t ^ (2 * j) for j in range(half)])
    whole = pl.BlockSpec((rows, width), lambda i, *_: (0, 0))
    column = pl.BlockSpec((model, tile), lambda i, *_: (0, jnp.minimum(i, tiles - 1)))
    grid_spec = pltpu.PrefetchScalarGridSpec(
        num_scalar_prefetch=2,
        grid=(tiles + 2 * half,),
        in_specs=[whole] * (2 * half)
        + [
            column,
            column,
            pl.BlockSpec(
                (units, width), lambda i, order, dest: (0, dest[jnp.maximum(i - tiles, 0)])
            ),
        ],
        out_specs=[
            pl.BlockSpec((1, rows, width), lambda i, *_: (jnp.clip(i - tiles, 0, half - 1), 0, 0)),
            pl.BlockSpec((1, rows, width), lambda i, *_: (jnp.clip(i - tiles - half, 0, half - 1), 0, 0)),
        ],
        scratch_shapes=[
            pltpu.VMEM((rows, model), jnp.bfloat16),
            pltpu.VMEM((rows, units), jnp.bfloat16),
        ],
    )
    shape = jax.ShapeDtypeStruct((half, rows, width), jnp.bfloat16)
    return pl.pallas_call(
        functools.partial(expert_kernel, tiles, half),
        grid_spec=grid_spec,
        out_shape=[shape, shape],
        name="experts",
    )(tp_order(), dest, *parts, gate_local, up_local, down_local)


def combine_kernel(offsets, ids_ref, route_ref, *refs):
    blocks, out_ref = refs[:-1], refs[-1]
    rows, chosen = ids_ref.shape
    experts = len(offsets)
    capacity = blocks[0].shape[0]
    expert = lax.broadcasted_iota(jnp.int32, (rows, experts), 1)
    picked = jnp.zeros((rows, experts), jnp.float32)
    weight = jnp.zeros((rows, experts), jnp.float32)
    for k in range(chosen):
        match = ids_ref[:, k : k + 1] == expert
        picked += jnp.where(match, 1.0, 0.0)
        weight += jnp.where(match, route_ref[:, k : k + 1], 0.0)
    earlier = lax.broadcasted_iota(jnp.int32, (rows, rows), 1) < lax.broadcasted_iota(
        jnp.int32, (rows, rows), 0
    )
    rank = dot32(jnp.where(earlier, 1.0, 0.0).astype(jnp.bfloat16), picked.astype(jnp.bfloat16))
    slot = jnp.where(picked > 0, rank, -1.0).astype(jnp.int32)
    place = lax.broadcasted_iota(jnp.int32, (rows, capacity), 1)
    total = None
    for d, block in zip(offsets, blocks):
        spread = jnp.where(place == slot[:, d : d + 1], weight[:, d : d + 1], 0.0)
        high = spread.astype(jnp.bfloat16)
        low = (spread - high.astype(jnp.float32)).astype(jnp.bfloat16)
        term = dot32(high, block[...]) + dot32(low, block[...])
        total = term if total is None else total + term
    out_ref[...] = total.astype(out_ref.dtype)


def expert_block(
    routed_in,
    routed_gain,
    expert_ids,
    group_logits,
    inner_logits,
    gate_weight,
    up_weight,
    down_weight,
):
    token_count = routed_in.shape[0]
    chosen = expert_ids.shape[1]
    ep_size = lax.axis_size("ep")
    capacity = 2 * chosen * token_count // ep_size
    width = routed_in.shape[1] // lax.axis_size("tp")
    index = lax.axis_index("ep").astype(jnp.int32)
    relative = jnp.where(expert_ids < index, expert_ids - index + ep_size, expert_ids - index)
    offsets = sorted(range(ep_size), key=lambda d: (min(d, ep_size - d), d))
    outgoing = pl.pallas_call(
        functools.partial(dispatch_kernel, offsets, capacity),
        in_specs=[SMEM, VMEM, VMEM, VMEM],
        out_specs=[VMEM] * ep_size,
        out_shape=[jax.ShapeDtypeStruct((capacity, width), jnp.bfloat16)] * ep_size,
        name="dispatch",
    )(
        lax.axis_index("tp").astype(jnp.int32)[None],
        relative.T,
        routed_gain[None, :],
        routed_in,
    )
    arrived = [x if d == 0 else shift(x, d) for d, x in zip(offsets, outgoing)]
    half = ep_size // 2
    returned = []
    for start in range(0, ep_size, half):
        batch = jnp.concatenate(arrived[start : start + half], axis=0)
        shares = tp_pieces(batch)
        send, keep = run_experts(shares, gate_weight[0], up_weight[0], down_weight[0])
        answered = add_shares(send, keep)
        for j, d in enumerate(offsets[start : start + half]):
            piece = answered[j * capacity : (j + 1) * capacity]
            returned.append(piece if d == 0 else shift(piece, ep_size - d))
    group_prob = jax.nn.softmax(group_logits, axis=-1)
    member = (
        expert_ids[..., None] // GROUP_SIZE == jnp.arange(group_logits.shape[1], dtype=jnp.int32)
    ).astype(jnp.float32)
    group_pick = jnp.sum(group_prob[:, None, :] * member, axis=-1)
    route_weight = group_pick * jax.nn.softmax(inner_logits, axis=-1)
    return pl.pallas_call(
        functools.partial(combine_kernel, offsets),
        in_specs=[VMEM] * (2 + ep_size),
        out_specs=VMEM,
        out_shape=jax.ShapeDtypeStruct((token_count, width), jnp.bfloat16),
        name="combine",
    )(relative, route_weight, *returned)


def local(
    queries,
    key_rows,
    values,
    second_scale,
    head_gain,
    out_weight,
    routed_in,
    routed_gain,
    expert_ids,
    group_logits,
    inner_logits,
    gate_weight,
    up_weight,
    down_weight,
):
    routed_out = expert_block(
        routed_in,
        routed_gain,
        expert_ids,
        group_logits,
        inner_logits,
        gate_weight,
        up_weight,
        down_weight,
    )
    mixer_out = token_mixer(queries, key_rows, values, second_scale, head_gain, out_weight)
    return (mixer_out, routed_out)


def solution(mesh):
    return jax.shard_map(
        local,
        mesh=mesh,
        in_specs=(
            P("ep", "tp"),
            P("ep", "tp"),
            P("ep", "tp"),
            P("tp"),
            P(),
            P(None, "tp"),
            P("ep", None),
            P(),
            P("ep", None),
            P("ep", None),
            P("ep", None),
            P("ep", None, "tp"),
            P("ep", None, "tp"),
            P("ep", "tp", None),
        ),
        out_specs=(P("ep", "tp"), P("ep", "tp")),
        check_vma=False,
    )
```
